256 devices in a mesh: sp: 64 (over z, x, core), tp: 4 (over y).
Axes of the slice: x: 4, y: 4, z: 8, core: 2. Of those that a mesh axis runs over, the one named last changes fastest.
Arguments:
- stream: bfloat16 [32768, 2048], P(('sp', 'tp')), may hold values from -6 to 6
- pool_in: bfloat16 [32768, 1024], P('sp', 'tp'), may hold values from -6 to 6
- doc_ids: int32 [32768], P('sp'), may hold values from 0 to 7, never falling along the last dimension, each value on 1 to 8192 neighbouring positions
- pool_map: bfloat16 [4, 256, 512], P('tp'), may hold values from -0.375 to 0.375
- pool_scale: float32 [2048], P('tp'), may hold values from 0.1 to 1.9
- out_weight: bfloat16 [2048, 2048], P('tp'), may hold values from -0.125 to 0.125
- norm_gain: float32 [2048], replicated, may hold values from 0.1 to 1.9
- routes: int32 [32768, 2], P('sp'), may hold values from 0 to 63, all different within a row; in each aligned block of 128 rows (0 to 127, 128 to 255, ...) at most 6 rows name the same one
- route_weight: float32 [32768, 2], P(('sp', 'tp')), may hold values from 0.2 to 1
- expert_gate: bfloat16 [64, 2048, 1024], P('sp', None, 'tp'), may hold values from -0.125 to 0.125
- expert_up: bfloat16 [64, 2048, 1024], P('sp', None, 'tp'), may hold values from -0.125 to 0.125
- expert_down: bfloat16 [64, 1024, 2048], P('sp', 'tp'), may hold values from -0.1875 to 0.1875
Outputs:
- result: bfloat16 [32768, 2048], P(('sp', 'tp'))
The draws below stay inside these ranges and needn't reach their ends.
Inputs may be any that keep to these rules, and one draw needn't show every extreme that they name: `routes`: each token names 2 different experts; in each aligned block of 128 rows no expert is named by more than 6 rows, a bound that some block reaches. `doc_ids`: never falling; each document holds at most 8192 positions.
All inputs are finite; a program needn't handle non-finite values.
Results may differ from the reference program's by a relative error of at most 0.014.
Values may be sent and summed in bfloat16 or wider, within the bound.
No kernel may reach another device: no remote copies, remote signals or barrier semaphores. Data moves between devices by JAX's collectives and lax.ppermute only.
A program may use at most 64 MiB of HBM per device.

```python
import math
import jax
import jax.numpy as jnp
import numpy as np
from jax import lax

D = 2048
PW = 1024
GROUPS = 4
FF = 1024
TOPK = 2
DOC_COUNT = 8
GW = 256
GOUT = 512
QUART = 128
TOKENS = 32768
EXPERTS = 64
CAP = 6
FF_PART = 256
DOC_MOST = 8192
N_TP = 4


def block_levels(rng, dims, cuts, low, high):
    loudness, own = 1.0, jax.random.fold_in(rng, 6)
    for dim, blocks in cuts:
        heights = jnp.exp(jax.random.uniform(jax.random.fold_in(own, dim), (blocks,), jnp.float32, low / len(cuts), high / len(cuts)))
        loudness = loudness * jnp.repeat(heights, dims[dim] // blocks).reshape([-1 if axis == dim else 1 for axis in range(len(dims))])
    return loudness


def split_up(number_of, total, bound, lean):
    loads = [(1 << 20) // math.isqrt(rank ** lean) + 1 for rank in range(2, number_of + 1)]
    spare, holding = total - bound - (number_of - 1), [1] * (number_of - 1)
    while spare > 0:
        candidates = [i for i in range(number_of - 1) if holding[i] < bound]
        pool, budget = sum([loads[i] for i in candidates]), spare
        for i in candidates:
            addition = min(bound - holding[i], max(1, budget * loads[i] // pool), spare)
            holding[i] = holding[i] + addition
            spare = spare - addition
    return np.array([bound] + holding)


def ragged_sizes(stream_key, number_of, total, reach, lean):
    if number_of == 2:
        one = jax.random.randint(stream_key, (), max(1, total - reach), min(reach, total - 1) + 1)
        return jnp.stack([one, total - one])
    lengths = jnp.asarray(split_up(number_of, total, reach, lean), jnp.int32)
    twos = (number_of - 1) // 2
    donor, receiver = lengths[1:1 + 2 * twos:2], lengths[2:2 + 2 * twos:2]
    slack = jnp.minimum(donor - 1, reach - receiver)
    passed = jax.random.randint(jax.random.fold_in(stream_key, 1), (twos,), 0, 1 << 20) % (slack + 1)
    lengths = lengths.at[1:1 + 2 * twos:2].set(donor - passed).at[2:2 + 2 * twos:2].set(receiver + passed)
    return lengths[jax.random.permutation(jax.random.fold_in(stream_key, 2), number_of)]


def routed_block(rng, own, number, rows, number_of, top, most, skew):
    order = jax.random.permutation(rng, number_of)
    heavy_load, usual = shares(number_of, rows * top, most, skew, True), shares(number_of, rows * top, most, skew, False)
    places = jnp.arange(number_of)

    def named(tallies, rotation):
        used = int((tallies > 0).sum())
        fixed = max(1, used // 4)
        moved = fixed + (places - fixed + rotation * (used - fixed)) % max(1, number_of - fixed)
        return jnp.zeros((number_of,), jnp.int32).at[order[jnp.where(places < fixed, places, moved)]].set(jnp.asarray(tallies, jnp.int32))

    tallies = jnp.where(number % 4 == 0, named(heavy_load, number // 4), named(usual, number - number // 4 - 1))
    mixed = jax.random.permutation(jax.random.fold_in(own, 3), number_of)
    giver, sink = mixed[0:number_of // 2 * 2:2], mixed[1:number_of // 2 * 2:2]
    margin = jnp.minimum(tallies[giver] - 1, most - tallies[sink]) // 2
    margin = jnp.where((giver == order[0]) | (sink == order[0]) | (tallies[sink] == 0), 0, jnp.maximum(margin, 0))
    moved = jax.random.randint(jax.random.fold_in(own, 4), (number_of // 2,), 0, 1 << 20) % (margin + 1)
    tallies = tallies.at[giver].add(-moved).at[sink].add(moved)
    items = jnp.searchsorted(jnp.cumsum(tallies), jnp.arange(rows * top), side="right").astype(jnp.int32)
    grid = items.reshape(top, rows).T
    grid = grid[jax.random.permutation(jax.random.fold_in(own, 1), rows)]
    rotation = jax.random.randint(jax.random.fold_in(own, 2), (rows, 1), 0, top)
    return jnp.take_along_axis(grid, (jnp.arange(top)[None, :] + rotation) % top, axis=1)


def shares(number_of, total, bound, skew, full):
    portions = [(1 << 20) // math.isqrt(grade ** skew) + 1 for grade in range(1, number_of + 1)]
    largest = bound if full else min(bound, max(-(-total // number_of), total * portions[0] // sum(portions)))
    least = 1 if total - largest >= number_of - 1 else 0
    given, rest = [largest] + [least] * (number_of - 1), total - largest - least * (number_of - 1)
    while rest > 0:
        movable = [i for i in range(1, number_of) if given[i] < largest] or [i for i in range(1, number_of) if given[i] < bound]
        whole, left = sum([portions[i] for i in movable]), rest
        for i in movable:
            more = min(bound - given[i], max(1, left * portions[i] // whole), rest)
            given[i] = given[i] + more
            rest = rest - more
    return np.array(given)


def normal_values(stream_key, shape, width, limit, pieces=(), kind=jnp.bfloat16):
    drawn = width * jax.random.normal(stream_key, shape, jnp.float32)
    if pieces:
        drawn = drawn * block_levels(stream_key, shape, pieces, -0.22, 0.18)
    return jnp.clip(drawn, -limit, limit).astype(kind)


def setup_inputs(seed: int = 0) -> dict:
    streams_of = jax.random.split(jax.random.key(seed), 13)
    stream = normal_values(streams_of[0], (TOKENS, D), 1.0, 6.0, ((0, 256),))
    pool_in = normal_values(streams_of[1], (TOKENS, PW), 1.0, 6.0, ((0, 64), (1, 4)))
    doc_ids = jnp.searchsorted(jnp.cumsum(ragged_sizes(streams_of[2], DOC_COUNT, TOKENS, DOC_MOST, 1)), jnp.arange(TOKENS), side="right").astype(jnp.int32)
    pool_map = normal_values(streams_of[3], (GROUPS, GW, GOUT), GW ** -0.5, 0.375, ((0, 4),))
    pool_scale = jnp.clip(1.0 + 0.18 * jax.random.normal(streams_of[4], (D,), jnp.float32), 0.1, 1.9)
    out_weight = normal_values(streams_of[5], (D, D), D ** -0.5, 0.125, ((0, 4),))
    norm_gain = jnp.clip(1.0 + 0.18 * jax.random.normal(streams_of[6], (D,), jnp.float32), 0.1, 1.9)
    routes_keys = jax.random.split(jax.random.fold_in(streams_of[7], 1), TOKENS // QUART)
    routes_turns = jax.random.permutation(jax.random.fold_in(streams_of[7], 3), TOKENS // QUART)
    routes = jax.vmap(lambda own, number: routed_block(jax.random.fold_in(streams_of[7], 2), own, number, QUART, EXPERTS, TOPK, CAP, 1))(routes_keys, routes_turns).reshape((TOKENS, TOPK))
    route_weight = jnp.clip(0.2 + 0.8 * jax.random.uniform(streams_of[8], (TOKENS, TOPK), jnp.float32) ** block_levels(streams_of[8], (TOKENS, TOPK), ((0, 256),), -0.2, 0.2), 0.2, 1.0)
    expert_gate = normal_values(streams_of[9], (EXPERTS, D, FF), D ** -0.5, 0.125, ((0, 64), (2, 4)))
    expert_up = normal_values(streams_of[10], (EXPERTS, D, FF), D ** -0.5, 0.125, ((0, 64), (2, 4)))
    expert_down = normal_values(streams_of[11], (EXPERTS, FF, D), FF ** -0.5, 0.1875, ((0, 64), (1, 4)))
    return dict(stream=stream, pool_in=pool_in, doc_ids=doc_ids, pool_map=pool_map, pool_scale=pool_scale, out_weight=out_weight, norm_gain=norm_gain, routes=routes, route_weight=route_weight, expert_gate=expert_gate, expert_up=expert_up, expert_down=expert_down)


EPS = 1e-06

def reference(stream, pool_in, doc_ids, pool_map, pool_scale, out_weight, norm_gain, routes, route_weight, expert_gate, expert_up, expert_down):
    total_rows = pool_in.shape[0]
    positions = jnp.arange(total_rows, dtype=jnp.int32)
    starts_here = jnp.concatenate([jnp.ones((1,), jnp.bool_), doc_ids[1:] != doc_ids[:-1]])
    doc_start = lax.cummax(jnp.where(starts_here, positions, 0).astype(jnp.int32), axis=0)
    source_rows = pool_in.astype(jnp.float32)
    branch_parts = []
    for group_index in range(GROUPS):
        window = 2 << group_index
        group_cols = source_rows[:, group_index * GW:(group_index + 1) * GW]
        running = jnp.zeros_like(group_cols)
        counts = jnp.zeros((total_rows,), jnp.float32)
        for offset in range(window):
            shifted = jnp.concatenate([jnp.zeros((offset, GW), jnp.float32), group_cols[:total_rows - offset]], axis=0)
            in_window = positions - offset >= doc_start
            running = running + jnp.where(in_window[:, None], shifted, 0.0)
            counts = counts + in_window.astype(jnp.float32)
        pooled = (running / counts[:, None] - group_cols).astype(jnp.bfloat16)
        mapped = jnp.dot(pooled, pool_map[group_index], preferred_element_type=jnp.float32)
        branch_parts.append((mapped * pool_scale[group_index * GOUT:(group_index + 1) * GOUT]).astype(jnp.bfloat16))
    branch = jnp.concatenate(branch_parts, axis=1)
    mixed_rows = (stream.astype(jnp.float32) + jnp.dot(branch, out_weight, preferred_element_type=jnp.float32)).astype(jnp.bfloat16)
    mixed_up = mixed_rows.astype(jnp.float32)
    normed = (mixed_up * lax.rsqrt(lax.optimization_barrier(jnp.mean(mixed_up * mixed_up, axis=1, keepdims=True)) + EPS) * norm_gain).astype(jnp.bfloat16)
    block_count = total_rows // QUART
    flattened = routes.reshape(-1).astype(jnp.int32)
    one_hot = (flattened[:, None] == jnp.arange(EXPERTS, dtype=jnp.int32)[None, :]).astype(jnp.int32)
    blocked = one_hot.reshape(block_count, QUART * TOPK, EXPERTS)
    ranking = lax.optimization_barrier(jnp.sum((jnp.cumsum(blocked, axis=1) - blocked) * blocked, axis=2)).reshape(-1).astype(jnp.int32)
    assign_ids = jnp.arange(total_rows * TOPK, dtype=jnp.int32)
    block_ids = (assign_ids // (QUART * TOPK)).astype(jnp.int32)
    target_slot = ((flattened * block_count + block_ids) * CAP + ranking).astype(jnp.int32)
    per_expert = block_count * CAP
    slot_token = jnp.zeros((EXPERTS * per_expert,), jnp.int32).at[target_slot].set((assign_ids // TOPK).astype(jnp.int32))
    slot_weight = jnp.zeros((EXPERTS * per_expert,), jnp.float32).at[target_slot].set(route_weight.reshape(-1))

    def one_expert(accumulated, expert_index):
        begin_slot = (expert_index * per_expert).astype(jnp.int32)
        tokens_here = lax.dynamic_slice_in_dim(slot_token, begin_slot, per_expert)
        weights_here = lax.dynamic_slice_in_dim(slot_weight, begin_slot, per_expert)
        inputs = normed[tokens_here]
        gate_pre = jnp.dot(inputs, expert_gate[expert_index], preferred_element_type=jnp.float32)
        up_pre = jnp.dot(inputs, expert_up[expert_index], preferred_element_type=jnp.float32)
        hidden = (jax.nn.silu(gate_pre) * up_pre).astype(jnp.bfloat16)
        down_rows = expert_down[expert_index]
        summed = jnp.zeros((per_expert, D), jnp.float32)
        for part_index in range(N_TP):
            part_begin = part_index * FF_PART
            part_out = jnp.dot(hidden[:, part_begin:part_begin + FF_PART], down_rows[part_begin:part_begin + FF_PART], preferred_element_type=jnp.float32).astype(jnp.bfloat16)
            summed = summed + lax.optimization_barrier(part_out).astype(jnp.float32)
        expert_out = lax.optimization_barrier(summed.astype(jnp.bfloat16)).astype(jnp.float32)
        return (accumulated.at[tokens_here].add(weights_here[:, None] * expert_out), None)
    accumulated, unused_out = lax.scan(one_expert, jnp.zeros((total_rows, D), jnp.float32), jnp.arange(EXPERTS, dtype=jnp.int32))
    return (mixed_up + accumulated).astype(jnp.bfloat16)
```

```python
import jax
import jax.numpy as jnp
from jax import lax
from jax.sharding import PartitionSpec as P

SPAN = 16


EPS = 1e-06


def passed_along(value, axis, by):
    length = lax.axis_size(axis)
    pairs = [(i, i + by) for i in range(length) if 0 <= i + by < length]
    return lax.ppermute(value, axis, pairs)


def cut_along(value, dim, length):
    before, after = (value.shape[:dim], value.shape[dim + 1 :])
    return jnp.moveaxis(value.reshape(*before, length, -1, *after), dim, 0)


def sum_at_owner(value, axis, dim):
    length = lax.axis_size(axis)
    tiles = lax.all_to_all(cut_along(value, dim, length), axis, 0, 0, tiled=True)
    return jnp.sum(tiles.astype(jnp.float32), axis=0)


def slot_table(route_block, expert_count, capacity, top_count):
    flattened = route_block.reshape(-1)
    one_hot = (flattened[:, None] == jnp.arange(expert_count, dtype=jnp.int32)[None, :]).astype(
        jnp.int32
    )
    ranking = jnp.sum((jnp.cumsum(one_hot, axis=0) - one_hot) * one_hot, axis=1)
    target_slot = flattened * capacity + ranking
    matches = target_slot[None, :] == jnp.arange(expert_count * capacity, dtype=jnp.int32)[:, None]
    sources = jnp.sum(
        jnp.where(matches, jnp.arange(flattened.shape[0], dtype=jnp.int32)[None, :], 0), axis=1
    )
    filled = jnp.any(matches, axis=1)
    return (target_slot, sources // top_count, filled)


def per_device(
    stream,
    pool_in,
    doc_ids,
    pool_map,
    pool_scale,
    out_weight,
    norm_gain,
    routes,
    route_weight,
    expert_gate,
    expert_up,
    expert_down,
):
    row_count = pool_in.shape[0]
    model_width = stream.shape[1]
    top_count = routes.shape[1]
    tp_count = lax.axis_size("tp")
    expert_count = lax.axis_size("sp")
    quarter = row_count // tp_count
    capacity = max(2, 3 * top_count * quarter // (2 * expert_count))
    reach_rows = SPAN - 1
    tail_rows = (
        pool_in[row_count - reach_rows :],
        doc_ids[row_count - reach_rows :].astype(jnp.bfloat16),
    )
    prior_rows, prior_docs = passed_along((tail_rows[0], tail_rows[1]), "sp", 1)
    extended = jnp.concatenate([prior_rows, pool_in], axis=0).astype(jnp.float32)
    extended_docs = jnp.concatenate([prior_docs.astype(jnp.float32), doc_ids.astype(jnp.float32)])
    own_docs = doc_ids.astype(jnp.float32)
    window = jnp.left_shift(jnp.int32(2), lax.axis_index("tp"))
    positions = lax.axis_index("sp") * row_count + jnp.arange(row_count, dtype=jnp.int32)
    running = jnp.zeros(pool_in.shape, jnp.float32)
    counts = jnp.zeros((row_count,), jnp.float32)
    for offset in range(reach_rows + 1):
        begin_row = reach_rows - offset
        piece_rows = extended[begin_row : begin_row + row_count]
        piece_docs = extended_docs[begin_row : begin_row + row_count]
        in_window = (offset < window) & (positions - offset >= 0) & (piece_docs == own_docs)
        running = running + jnp.where(in_window[:, None], piece_rows, 0.0)
        counts = counts + in_window.astype(jnp.float32)
    pooled = (running / counts[:, None] - pool_in.astype(jnp.float32)).astype(jnp.bfloat16)
    branch = (jnp.dot(pooled, pool_map[0], preferred_element_type=jnp.float32) * pool_scale).astype(
        jnp.bfloat16
    )
    projected = sum_at_owner(
        jnp.dot(branch, out_weight, preferred_element_type=jnp.float32).astype(jnp.bfloat16),
        "tp",
        0,
    )
    mixed_rows = (stream.astype(jnp.float32) + projected).astype(jnp.bfloat16)
    mixed_up = mixed_rows.astype(jnp.float32)
    normed = (
        mixed_up * lax.rsqrt(jnp.mean(mixed_up * mixed_up, axis=1, keepdims=True) + EPS) * norm_gain
    ).astype(jnp.bfloat16)
    own_routes = lax.dynamic_slice_in_dim(routes, lax.axis_index("tp") * quarter, quarter, 0)
    own_slots, own_sources, own_filled = slot_table(own_routes, expert_count, capacity, top_count)
    token_index = own_sources.reshape(expert_count, capacity)
    lanes = 128
    rows3 = normed.reshape(quarter, model_width // lanes, lanes)
    dispatch = rows3[token_index]
    arrived = lax.all_to_all(dispatch, "sp", split_axis=0, concat_axis=0, tiled=True)
    stacked = arrived.reshape(-1, model_width)
    gates = lax.all_gather(expert_gate[0], "tp", axis=0, tiled=False)
    ups = lax.all_gather(expert_up[0], "tp", axis=0, tiled=False)
    downs = lax.all_gather(expert_down[0], "tp", axis=0, tiled=False)
    summed = jnp.zeros(stacked.shape, jnp.float32)
    for part in range(tp_count):
        gate_pre = jnp.dot(stacked, gates[part], preferred_element_type=jnp.float32)
        up_pre = jnp.dot(stacked, ups[part], preferred_element_type=jnp.float32)
        hidden = (jax.nn.silu(gate_pre) * up_pre).astype(jnp.bfloat16)
        summed = summed + jnp.dot(hidden, downs[part], preferred_element_type=jnp.float32)
    expert_out = summed.astype(jnp.bfloat16).reshape(arrived.shape)
    returned = lax.all_to_all(expert_out, "sp", split_axis=0, concat_axis=0, tiled=True)
    outputs = returned.reshape(expert_count * capacity, model_width // lanes, lanes)
    picked = outputs[own_slots].astype(jnp.float32).reshape(quarter, top_count, model_width // lanes, lanes)
    combined = jnp.sum(route_weight[:, :, None, None] * picked, axis=1).reshape(quarter, model_width)
    return (mixed_up + combined).astype(jnp.bfloat16)


def solution(mesh):
    in_specs = (
        P(("sp", "tp"), None),
        P("sp", "tp"),
        P("sp"),
        P("tp", None, None),
        P("tp"),
        P("tp", None),
        P(),
        P("sp", None),
        P(("sp", "tp"), None),
        P("sp", None, "tp"),
        P("sp", None, "tp"),
        P("sp", "tp", None),
    )
    out_specs = P(("sp", "tp"), None)
    return jax.shard_map(
        per_device, mesh=mesh, in_specs=in_specs, out_specs=out_specs, check_vma=False
    )
```

```python
import functools

import jax
import jax.numpy as jnp
from jax import lax
from jax.experimental import pallas as pl
from jax.experimental.pallas import tpu as pltpu
from jax.sharding import Mesh, PartitionSpec as P

SPAN = 16
EPS = 1e-06
LANES = 128


VMEM = pl.BlockSpec(memory_space=pltpu.VMEM)
SMEM = pl.BlockSpec(memory_space=pltpu.SMEM)
HBM = pl.BlockSpec(memory_space=pltpu.HBM)


def dispatch_kernel(rows, width, slots, tok_ref, parts_ref, stream_ref, gain_ref, out_ref, mixed_ref, wide, tiles):
    chunks = width // LANES
    total = stream_ref[...].astype(jnp.float32)
    own = parts_ref[0].astype(jnp.float32)
    for part in range(1, parts_ref.shape[0]):
        own = own + parts_ref[part].astype(jnp.float32)
    mixed = (total + own).astype(jnp.bfloat16)
    mixed_ref[...] = mixed
    up = mixed.astype(jnp.float32)
    scale = lax.rsqrt(jnp.sum(up * up, axis=1, keepdims=True) * (1.0 / width) + EPS)
    for chunk in range(chunks):
        cols = slice(chunk * LANES, (chunk + 1) * LANES)
        piece = up[:, cols] * scale * gain_ref[:, cols]
        wide[pl.ds(chunk, rows, stride=chunks), :] = piece
    tiles[...] = wide[...].astype(jnp.bfloat16).reshape(rows, chunks, LANES)

    @pl.loop(0, slots, unroll=8)
    def _(slot):
        out_ref[slot] = tiles[tok_ref[slot]]


def hidden_kernel(rows, width, ff, half, x_ref, *refs):
    w_refs = refs[:10]
    out_ref, wide, flat = refs[10:]
    chunks = width // LANES
    is_home = half()
    wide[...] = x_ref[...].astype(jnp.float32)
    for chunk in range(chunks):
        flat[:, chunk * LANES : (chunk + 1) * LANES] = wide[pl.ds(chunk, rows, stride=chunks), :].astype(jnp.bfloat16)

    def fill(place, gate_ref, up_ref):
        gate_pre = jnp.dot(flat[...], gate_ref[...], preferred_element_type=jnp.float32)
        up_pre = jnp.dot(flat[...], up_ref[...], preferred_element_type=jnp.float32)
        hidden = gate_pre / (1.0 + jnp.exp(-gate_pre)) * up_pre
        out_ref[:, place * ff : (place + 1) * ff] = hidden.astype(jnp.bfloat16)

    @pl.when(is_home == 1)
    def _():
        fill(0, w_refs[0], w_refs[1])

    @pl.when(is_home == 0)
    def _():
        fill(0, w_refs[2], w_refs[3])

    for place in range(1, 4):
        fill(place, w_refs[2 + 2 * place], w_refs[3 + 2 * place])


def down_kernel(rows, width, ff, half, hidden_ref, *refs):
    own_ref, late_ref = refs[:2]
    w_refs = refs[2:5]
    out_ref, wide, first = refs[5:]
    chunks = width // LANES
    is_home = half()

    @pl.when(is_home == 1)
    def _():
        first[...] = own_ref[...]

    @pl.when(is_home == 0)
    def _():
        first[...] = late_ref[...]

    step = 2 * LANES
    for begin in range(0, width, step):
        cols = slice(begin, begin + step)
        total = jnp.dot(hidden_ref[:, :ff], first[:, cols], preferred_element_type=jnp.float32)
        for place in range(1, 4):
            total = total + jnp.dot(
                hidden_ref[:, place * ff : (place + 1) * ff],
                w_refs[place - 1][:, cols],
                preferred_element_type=jnp.float32,
            )
        for piece in range(2):
            wide[pl.ds(begin // LANES + piece, rows, stride=chunks), :] = total[:, piece * LANES : (piece + 1) * LANES]
    out_ref[...] = wide[...].astype(jnp.bfloat16)


def combine_kernel(rows, width, top, pos_ref, weight_ref, got_ref, mixed_ref, out_ref, wide):
    chunks = width // LANES

    @pl.loop(0, rows, unroll=4)
    def _(row):
        total = weight_ref[row * top] * got_ref[pos_ref[row * top]].astype(jnp.float32)
        for k in range(1, top):
            total = total + weight_ref[row * top + k] * got_ref[pos_ref[row * top + k]].astype(jnp.float32)
        wide[pl.ds(row * chunks, chunks), :] = total

    for chunk in range(chunks):
        cols = slice(chunk * LANES, (chunk + 1) * LANES)
        piece = wide[pl.ds(chunk, rows, stride=chunks), :]
        out_ref[:, cols] = (mixed_ref[:, cols].astype(jnp.float32) + piece).astype(jnp.bfloat16)


def slot_tables(route_block, expert_count, capacity, top_count):
    flattened = route_block.reshape(-1)
    one_hot = (flattened[:, None] == jnp.arange(expert_count, dtype=jnp.int32)[None, :]).astype(jnp.int32)
    ranking = jnp.sum((jnp.cumsum(one_hot, axis=0) - one_hot) * one_hot, axis=1)
    side = capacity // 2
    place = ((flattened // 2 * 2 + ranking // side) * 2 + flattened % 2) * side + ranking % side
    matches = place[None, :] == jnp.arange(expert_count * capacity, dtype=jnp.int32)[:, None]
    sources = jnp.sum(jnp.where(matches, jnp.arange(flattened.shape[0], dtype=jnp.int32)[None, :], 0), axis=1)
    return place, sources // top_count


def weight_moves(sp_count, tp_count):
    def at(pair, core, y):
        return (2 * pair + core) * tp_count + y % tp_count

    pairs = [(pair, y) for pair in range(sp_count // 2) for y in range(tp_count)]
    home = lambda p, y: at(p, y % 2, y)
    away = lambda p, y: at(p, 1 - y % 2, y)
    over = [(home(p, y), away(p, y)) for p, y in pairs]
    back = [(away(p, y), home(p, y)) for p, y in pairs]
    plus = [(away(p, y), home(p, y + 1)) for p, y in pairs]
    minus = [(away(p, y), home(p, y - 1)) for p, y in pairs]
    far = [(home(p, y), away(p, y + 2)) for p, y in pairs]
    return plus + far, over + back, minus + over, over


ALL = ("sp", "yh", "yl")
TP = ("yh", "yl")


def forward(
    stream,
    pool_in,
    doc_ids,
    pool_map,
    pool_scale,
    out_weight,
    norm_gain,
    routes,
    route_weight,
    expert_gate,
    expert_up,
    expert_down,
):
    row_count = pool_in.shape[0]
    model_width = stream.shape[1]
    top_count = routes.shape[1]
    tp_count = lax.axis_size(TP)
    expert_count = lax.axis_size("sp")
    quarter = row_count // tp_count
    capacity = max(2, 3 * top_count * quarter // (2 * expert_count))
    slots = expert_count * capacity
    chunks = model_width // LANES
    reach_rows = SPAN - 1
    tp_index = lax.axis_index(TP)

    tail = jnp.concatenate(
        [
            pool_in[row_count - reach_rows :],
            jnp.pad(doc_ids[row_count - reach_rows :].astype(jnp.bfloat16), (0, pool_in.shape[1] - reach_rows))[None],
        ],
        axis=0,
    )
    prior = lax.ppermute(tail, "sp", [(i, i + 1) for i in range(expert_count - 1)])
    prior_rows, prior_docs = prior[:reach_rows], prior[reach_rows, :reach_rows]
    extended = jnp.concatenate([prior_rows, pool_in], axis=0).astype(jnp.float32)
    extended_docs = jnp.concatenate([prior_docs.astype(jnp.float32), doc_ids.astype(jnp.float32)])
    own_docs = doc_ids.astype(jnp.float32)
    window = jnp.left_shift(jnp.int32(2), tp_index)
    positions = lax.axis_index("sp") * row_count + jnp.arange(row_count, dtype=jnp.int32)
    running = jnp.zeros(pool_in.shape, jnp.float32)
    counts = jnp.zeros((row_count,), jnp.float32)
    for offset in range(reach_rows + 1):
        begin_row = reach_rows - offset
        piece_rows = extended[begin_row : begin_row + row_count]
        piece_docs = extended_docs[begin_row : begin_row + row_count]
        in_window = (offset < window) & (positions - offset >= 0) & (piece_docs == own_docs)
        running = running + jnp.where(in_window[:, None], piece_rows, 0.0)
        counts = counts + in_window.astype(jnp.float32)
    pooled = (running / counts[:, None] - pool_in.astype(jnp.float32)).astype(jnp.bfloat16)
    branch = (jnp.dot(pooled, pool_map[0], preferred_element_type=jnp.float32) * pool_scale).astype(jnp.bfloat16)
    partial = jnp.dot(branch, out_weight, preferred_element_type=jnp.float32).astype(jnp.bfloat16)
    partial = partial.reshape(tp_count, quarter, model_width)

    own = (expert_gate[0], expert_up[0], expert_down[0])
    ahead, swap, behind, over = weight_moves(expert_count, tp_count)
    parts = lax.all_to_all(partial, TP, 0, 0, tiled=True)
    held = []
    for array in own:
        first = lax.ppermute(array, ALL, ahead)
        second = lax.ppermute(array, ALL, behind)
        third = lax.ppermute(first, ALL, swap)
        fourth = lax.ppermute(second, ALL, over)
        held.append((array, fourth, second, first, third))

    own_routes = lax.dynamic_slice_in_dim(routes, tp_index * quarter, quarter, 0)
    places, tokens = slot_tables(own_routes, expert_count, capacity, top_count)

    dispatch, mixed_rows = pl.pallas_call(
        functools.partial(dispatch_kernel, quarter, model_width, slots),
        out_shape=(
            jax.ShapeDtypeStruct((slots, chunks, LANES), jnp.bfloat16),
            jax.ShapeDtypeStruct((quarter, model_width), jnp.bfloat16),
        ),
        in_specs=[SMEM, VMEM, VMEM, VMEM],
        out_specs=(VMEM, VMEM),
        scratch_shapes=[
            pltpu.VMEM((quarter * chunks, LANES), jnp.float32),
            pltpu.VMEM((quarter, chunks, LANES), jnp.bfloat16),
        ],
        name="dispatch",
    )(tokens, parts, stream, norm_gain[None])

    groups = expert_count * 2
    send = dispatch.reshape(groups, capacity // 2, chunks, LANES)
    arrived = lax.all_to_all(send, ("sp", "yl"), 0, 0, tiled=True)

    ff = expert_gate.shape[2]
    is_home = lambda: (lax.axis_index("sp") % 2 == lax.axis_index("yl")).astype(jnp.int32)
    hidden = pl.pallas_call(
        functools.partial(hidden_kernel, slots, model_width, ff, is_home),
        out_shape=jax.ShapeDtypeStruct((slots, ff * tp_count), jnp.bfloat16),
        in_specs=[VMEM] * 11,
        out_specs=VMEM,
        scratch_shapes=[
            pltpu.VMEM((slots * chunks, LANES), jnp.float32),
            pltpu.VMEM((slots, model_width), jnp.bfloat16),
        ],
        name="hidden",
    )(arrived.reshape(slots * chunks, LANES), *[h[i] for i in range(5) for h in held[:2]])
    expert_rows = pl.pallas_call(
        functools.partial(down_kernel, slots, model_width, ff, is_home),
        out_shape=jax.ShapeDtypeStruct((slots * chunks, LANES), jnp.bfloat16),
        in_specs=[VMEM] * 6,
        out_specs=VMEM,
        scratch_shapes=[
            pltpu.VMEM((slots * chunks, LANES), jnp.float32),
            pltpu.VMEM((ff, model_width), jnp.bfloat16),
        ],
        name="down",
    )(hidden, *held[2])

    returned = lax.all_to_all(
        expert_rows.reshape(groups, capacity // 2, chunks, LANES), ("sp", "yl"), 0, 0, tiled=True
    )
    return pl.pallas_call(
        functools.partial(combine_kernel, quarter, model_width, top_count),
        out_shape=jax.ShapeDtypeStruct((quarter, model_width), jnp.bfloat16),
        in_specs=[SMEM, SMEM, VMEM, VMEM],
        out_specs=VMEM,
        scratch_shapes=[pltpu.VMEM((quarter * chunks, LANES), jnp.float32)],
        name="combine",
    )(places, route_weight.reshape(-1), returned.reshape(slots, chunks, LANES), mixed_rows)


def solution(mesh):
    split = Mesh(mesh.devices.reshape(mesh.shape["sp"], mesh.shape["tp"] // 2, 2), ALL)
    in_specs = (
        P(ALL, None),
        P("sp", TP),
        P("sp"),
        P(TP, None, None),
        P(TP),
        P(TP, None),
        P(),
        P("sp", None),
        P(ALL, None),
        P("sp", None, TP),
        P("sp", None, TP),
        P("sp", TP, None),
    )
    return jax.shard_map(forward, mesh=split, in_specs=in_specs, out_specs=P(ALL, None), check_vma=False)
```

```python
import functools

import jax
import jax.numpy as jnp
from jax import lax
from jax.experimental import pallas as pl
from jax.experimental.pallas import tpu as pltpu
from jax.sharding import Mesh, PartitionSpec as P

SPAN = 16
EPS = 1e-06
LANES = 128


VMEM = pl.BlockSpec(memory_space=pltpu.VMEM)
SMEM = pl.BlockSpec(memory_space=pltpu.SMEM)
HBM = pl.BlockSpec(memory_space=pltpu.HBM)


def tile_rows(rows, chunk):
    return pl.ds(chunk // 8 * rows * 8 + chunk % 8, rows, stride=8)


def spread(wide, rows, chunks, value):
    tall = value.astype(jnp.float32).reshape(rows, chunks, LANES)
    for part in range(chunks // 8):
        wide[part * rows * 8 : (part + 1) * rows * 8] = tall[:, part * 8 : part * 8 + 8].reshape(rows * 8, LANES)


def gathered(wide, rows, chunks):
    parts = [wide[part * rows * 8 : (part + 1) * rows * 8].reshape(rows, 8, LANES) for part in range(chunks // 8)]
    return jnp.concatenate(parts, axis=1).astype(jnp.bfloat16)


def mix_kernel(rows, reach, pool_ref, docs_ref, prior_ref, map_ref, scale_ref, weight_ref, *refs):
    own_ref, far_plus, far_minus, next_low, next_high, prev_low, prev_high = refs[:7]
    data, docs, tally, turned = refs[7:]
    width = pool_ref.shape[1]
    tp = lax.axis_index(TP)
    window = jnp.left_shift(jnp.int32(2), tp)
    first = (lax.axis_index(SP) == 0).astype(jnp.float32)
    data[:reach] = jnp.zeros((reach, width), jnp.float32)
    data[reach : 2 * reach] = prior_ref[:, :width].astype(jnp.float32)
    data[2 * reach :] = pool_ref[...].astype(jnp.float32)
    docs[:reach] = jnp.full((reach, LANES), -1.0, jnp.float32)
    docs[reach : 2 * reach] = prior_ref[:, width:].astype(jnp.float32) * (1.0 - first) - first
    docs[2 * reach :] = docs_ref[...].astype(jnp.float32)
    tally[...] = jnp.ones(tally.shape, jnp.float32)
    extent = rows + reach
    span = 1
    while span < reach:
        @pl.when(span < window)
        def _():
            same = docs[reach:] == docs[reach - span : reach - span + extent]
            wide_same = jnp.concatenate([same] * (width // LANES), axis=1)
            grown = data[reach:] + jnp.where(wide_same, data[reach - span : reach - span + extent], 0.0)
            counted = tally[reach:] + jnp.where(same, tally[reach - span : reach - span + extent], 0.0)
            data[reach:] = grown
            tally[reach:] = counted

        span *= 2
    count = jnp.concatenate([tally[2 * reach :]] * (width // LANES), axis=1)
    pooled = (data[2 * reach :] / count - pool_ref[...].astype(jnp.float32)).astype(jnp.bfloat16)
    branch = (jnp.dot(pooled, map_ref[0], preferred_element_type=jnp.float32) * scale_ref[...]).astype(jnp.bfloat16)
    quarter = rows // 4
    turned[...] = branch
    order = [turned[pl.ds(lax.rem(tp + step, 4) * quarter, quarter), :] for step in range(4)]
    lined = jnp.concatenate(order, axis=0)
    half = weight_ref.shape[1] // 2
    low = jnp.dot(lined, weight_ref[:, :half], preferred_element_type=jnp.float32).astype(jnp.bfloat16)
    own_ref[:, :half] = low[:quarter]
    next_low[...] = low[quarter : 2 * quarter]
    far_minus[...] = low[2 * quarter : 3 * quarter]
    prev_low[...] = low[3 * quarter :]
    high = jnp.dot(lined, weight_ref[:, half:], preferred_element_type=jnp.float32).astype(jnp.bfloat16)
    own_ref[:, half:] = high[:quarter]
    next_high[...] = high[quarter : 2 * quarter]
    far_plus[...] = high[2 * quarter : 3 * quarter]
    prev_high[...] = high[3 * quarter :]


def dispatch_kernel(rows, width, slots, tok_ref, own_ref, nl_ref, nh_ref, pl_ref, ph_ref, stream_ref, gain_ref, out_ref, mixed_ref, wide, tiles):
    chunks = width // LANES
    low = nl_ref[...].astype(jnp.float32) + pl_ref[...].astype(jnp.float32)
    high = nh_ref[...].astype(jnp.float32) + ph_ref[...].astype(jnp.float32)
    total = own_ref[...].astype(jnp.float32) + jnp.concatenate([low, high], axis=1)
    mixed = (stream_ref[...].astype(jnp.float32) + total).astype(jnp.bfloat16)
    mixed_ref[...] = mixed
    up = mixed.astype(jnp.float32)
    scale = lax.rsqrt(jnp.sum(up * up, axis=1, keepdims=True) * (1.0 / width) + EPS)
    for chunk in range(chunks):
        cols = slice(chunk * LANES, (chunk + 1) * LANES)
        piece = up[:, cols] * scale * gain_ref[:, cols]
        wide[tile_rows(rows, chunk), :] = piece
    tiles[...] = gathered(wide, rows, chunks)

    @pl.loop(0, slots, unroll=8)
    def _(slot):
        out_ref[slot] = tiles[tok_ref[slot]]


def hidden_kernel(rows, width, ff, half, x_ref, *refs):
    own, late, near, both, other, last = [refs[2 * i : 2 * i + 2] for i in range(6)]
    out_ref, got, wide, flat, gates, ups, sems, got_sem = refs[12:]
    chunks = width // LANES
    is_home = half()
    home_side = (own, near, both, other)
    away_side = (late, near, both, last)
    targets = (gates, ups)

    got_copy = pltpu.make_async_copy(x_ref, got, got_sem)
    got_copy.start()

    def copy_in(side, place, j):
        return pltpu.make_async_copy(side[place][j], targets[j].at[place], sems.at[j, place])

    for place in range(4):
        for j in range(2):
            if home_side[place] is away_side[place]:
                copy_in(home_side, place, j).start()
            else:
                @pl.when(is_home == 1)
                def _():
                    copy_in(home_side, place, j).start()

                @pl.when(is_home == 0)
                def _():
                    copy_in(away_side, place, j).start()

    got_copy.wait()
    spread(wide, rows, chunks, got[...])
    for chunk in range(chunks):
        flat[:, chunk * LANES : (chunk + 1) * LANES] = wide[tile_rows(rows, chunk), :].astype(jnp.bfloat16)

    for place in range(4):
        copy_in(home_side, place, 0).wait()
        copy_in(home_side, place, 1).wait()
        gate_pre = jnp.dot(flat[...], gates[place], preferred_element_type=jnp.float32)
        up_pre = jnp.dot(flat[...], ups[place], preferred_element_type=jnp.float32)
        hidden = gate_pre / (1.0 + jnp.exp(-gate_pre)) * up_pre
        out_ref[:, place * ff : (place + 1) * ff] = hidden.astype(jnp.bfloat16)


def down_kernel(rows, width, ff, half, hidden_ref, *refs):
    own, late, near, both, other, last = refs[:6]
    out_ref, wide, downs, sems = refs[7:]
    chunks = width // LANES
    is_home = half()
    home_side = (own, near, both, other)
    away_side = (late, near, both, last)
    step = 4 * LANES

    def copy_in(side, place, begin):
        cols = pl.ds(begin, step)
        return pltpu.make_async_copy(
            side[place].at[:, cols], downs.at[pl.ds(place * ff, ff), cols], sems.at[place, begin // step]
        )

    for begin in range(0, width, step):
        for place in range(4):
            if home_side[place] is away_side[place]:
                copy_in(home_side, place, begin).start()
            else:
                @pl.when(is_home == 1)
                def _():
                    copy_in(home_side, place, begin).start()

                if place < 3:
                    @pl.when(is_home == 0)
                    def _():
                        copy_in(away_side, place, begin).start()

    @pl.when(is_home == 0)
    def _():
        downs[3 * ff :, :] = last[...]

    for begin in range(0, width, step):
        for place in range(3):
            copy_in(home_side, place, begin).wait()

        @pl.when(is_home == 1)
        def _():
            copy_in(home_side, 3, begin).wait()

        total = jnp.dot(hidden_ref[...], downs[:, begin : begin + step], preferred_element_type=jnp.float32)
        for piece in range(step // LANES):
            wide[tile_rows(rows, begin // LANES + piece), :] = total[:, piece * LANES : (piece + 1) * LANES]
    out_ref[...] = gathered(wide, rows, chunks)


def combine_kernel(rows, width, top, pos_ref, weight_ref, got_ref, mixed_ref, out_ref, wide):
    chunks = width // LANES

    @pl.loop(0, rows, unroll=4)
    def _(row):
        total = weight_ref[row * top] * got_ref[pos_ref[row * top]].astype(jnp.float32)
        for k in range(1, top):
            total = total + weight_ref[row * top + k] * got_ref[pos_ref[row * top + k]].astype(jnp.float32)
        for part in range(chunks // 8):
            wide[pl.ds(pl.multiple_of(part * rows * 8 + row * 8, 8), 8), :] = total[part * 8 : part * 8 + 8]

    for chunk in range(chunks):
        cols = slice(chunk * LANES, (chunk + 1) * LANES)
        piece = wide[tile_rows(rows, chunk), :]
        out_ref[:, cols] = (mixed_ref[:, cols].astype(jnp.float32) + piece).astype(jnp.bfloat16)


def slot_tables(route_block, expert_count, capacity, top_count, flip):
    flattened = route_block.reshape(-1)
    one_hot = (flattened[:, None] == jnp.arange(expert_count, dtype=jnp.int32)[None, :]).astype(jnp.int32)
    ranking = jnp.sum((jnp.cumsum(one_hot, axis=0) - one_hot) * one_hot, axis=1)
    place = (flattened // 2 * 2 + (flattened + flip) % 2) * capacity + ranking
    matches = place[None, :] == jnp.arange(expert_count * capacity, dtype=jnp.int32)[:, None]
    sources = jnp.sum(jnp.where(matches, jnp.arange(flattened.shape[0], dtype=jnp.int32)[None, :], 0), axis=1)
    return place, sources // top_count


def weight_moves(sp_count, tp_count):
    def at(pair, core, y):
        return (2 * pair + core) * tp_count + y

    served = lambda y: (y % 2 + y // 2) % 2
    home = lambda p, y: at(p, served(y), y)
    away = lambda p, y: at(p, 1 - served(y), y)
    inner = lambda y: tp_count - 1 - y
    outer = lambda y: y + 1 - 2 * (y % 2)
    pairs = [(pair, y) for pair in range(sp_count // 2) for y in range(tp_count)]
    over = [(home(p, y), away(p, y)) for p, y in pairs]
    back = [(away(p, y), home(p, y)) for p, y in pairs]
    near = [(home(p, y), home(p, inner(y))) for p, y in pairs] + [(away(p, y), away(p, outer(y))) for p, y in pairs]
    relay = [(away(p, y), home(p, inner(y))) for p, y in pairs] + over
    return near, relay, over, back


ALL = ("pair", "core", "yh", "yl")
SP = ("pair", "core")
TP = ("yh", "yl")


def forward(
    stream,
    pool_in,
    doc_ids,
    pool_map,
    pool_scale,
    out_weight,
    norm_gain,
    routes,
    route_weight,
    expert_gate,
    expert_up,
    expert_down,
):
    row_count = pool_in.shape[0]
    model_width = stream.shape[1]
    top_count = routes.shape[1]
    tp_count = lax.axis_size(TP)
    expert_count = lax.axis_size(SP)
    quarter = row_count // tp_count
    capacity = max(2, 3 * top_count * quarter // (2 * expert_count))
    slots = expert_count * capacity
    chunks = model_width // LANES
    tp_index = lax.axis_index(TP)
    docs = jnp.broadcast_to(doc_ids.astype(jnp.bfloat16)[:, None], (row_count, LANES))
    tail = jnp.concatenate([pool_in[row_count - SPAN :], docs[row_count - SPAN :]], axis=1)
    prior = lax.ppermute(tail, SP, [(i, i + 1) for i in range(expert_count - 1)])
    piece = jax.ShapeDtypeStruct((quarter, model_width // 2), jnp.bfloat16)
    held_rows, far_plus, far_minus, next_low, next_high, prev_low, prev_high = pl.pallas_call(
        functools.partial(mix_kernel, row_count, SPAN),
        out_shape=(jax.ShapeDtypeStruct((quarter, model_width), jnp.bfloat16),) + (piece,) * 6,
        in_specs=[VMEM] * 6,
        out_specs=(VMEM,) * 7,
        scratch_shapes=[
            pltpu.VMEM((row_count + 2 * SPAN, pool_in.shape[1]), jnp.float32),
            pltpu.VMEM((row_count + 2 * SPAN, LANES), jnp.float32),
            pltpu.VMEM((row_count + 2 * SPAN, LANES), jnp.float32),
            pltpu.VMEM((row_count, out_weight.shape[0]), jnp.bfloat16),
        ],
        name="mix",
    )(pool_in, docs, prior, pool_map, pool_scale[None], out_weight)

    own = (expert_gate[0], expert_up[0], expert_down[0])
    near, relay, over, back = weight_moves(expert_count, tp_count)
    plus = [(y, (y + 1) % tp_count) for y in range(tp_count)]
    minus = [(y, (y - 1) % tp_count) for y in range(tp_count)]

    def pass_on(array, pairs):
        return lax.ppermute(array, TP, pairs)

    def joined(left, right):
        return (left.astype(jnp.float32) + right.astype(jnp.float32)).astype(jnp.bfloat16)

    from_low = pass_on(far_plus, plus)
    from_high = pass_on(far_minus, minus)
    got_next_low = pass_on(next_low, plus)
    got_prev_high = pass_on(prev_high, minus)
    got_next_high = pass_on(joined(next_high, from_low), plus)
    got_prev_low = pass_on(joined(prev_low, from_high), minus)
    held = []
    for array in own:
        first = lax.ppermute(array, ALL, near)
        second = lax.ppermute(first, ALL, relay)
        late = lax.ppermute(array, ALL, over)
        other = lax.ppermute(first, ALL, back)
        last = lax.ppermute(second, ALL, over)
        held.append((array, late, first, second, other, last))

    own_routes = lax.dynamic_slice_in_dim(routes, tp_index * quarter, quarter, 0)
    places, tokens = slot_tables(own_routes, expert_count, capacity, top_count, lax.axis_index("yh"))

    dispatch, mixed_rows = pl.pallas_call(
        functools.partial(dispatch_kernel, quarter, model_width, slots),
        out_shape=(
            jax.ShapeDtypeStruct((slots, chunks, LANES), jnp.bfloat16),
            jax.ShapeDtypeStruct((quarter, model_width), jnp.bfloat16),
        ),
        in_specs=[SMEM] + [VMEM] * 7,
        out_specs=(VMEM, VMEM),
        scratch_shapes=[
            pltpu.VMEM((quarter * chunks, LANES), jnp.float32),
            pltpu.VMEM((quarter, chunks, LANES), jnp.bfloat16),
        ],
        name="dispatch",
    )(tokens, held_rows, got_next_low, got_next_high, got_prev_low, got_prev_high, stream, norm_gain[None])

    send = dispatch.reshape(expert_count, capacity, chunks, LANES)
    arrived = lax.all_to_all(send, ("pair", "yl"), 0, 0, tiled=True)

    ff = expert_gate.shape[2]
    flat_weight = route_weight.reshape(-1)
    is_home = lambda: (lax.axis_index("core") == (lax.axis_index("yl") + lax.axis_index("yh")) % 2).astype(jnp.int32)
    hidden = pl.pallas_call(
        functools.partial(hidden_kernel, slots, model_width, ff, is_home),
        out_shape=jax.ShapeDtypeStruct((slots, ff * tp_count), jnp.bfloat16),
        in_specs=[HBM] * 13,
        out_specs=VMEM,
        scratch_shapes=[
            pltpu.VMEM((slots * chunks, LANES), jnp.bfloat16),
            pltpu.VMEM((slots * chunks, LANES), jnp.float32),
            pltpu.VMEM((slots, model_width), jnp.bfloat16),
            pltpu.VMEM((tp_count, model_width, ff), jnp.bfloat16),
            pltpu.VMEM((tp_count, model_width, ff), jnp.bfloat16),
            pltpu.SemaphoreType.DMA((2, tp_count)),
            pltpu.SemaphoreType.DMA,
        ],
        name="hidden",
    )(arrived.reshape(slots * chunks, LANES), *[h[i] for i in range(6) for h in held[:2]])
    expert_rows = pl.pallas_call(
        functools.partial(down_kernel, slots, model_width, ff, is_home),
        out_shape=jax.ShapeDtypeStruct((slots, chunks, LANES), jnp.bfloat16),
        in_specs=[VMEM] + [HBM] * 5 + [VMEM, SMEM],
        out_specs=VMEM,
        scratch_shapes=[
            pltpu.VMEM((slots * chunks, LANES), jnp.float32),
            pltpu.VMEM((ff * tp_count, model_width), jnp.bfloat16),
            pltpu.SemaphoreType.DMA((tp_count, model_width // (4 * LANES))),
        ],
        compiler_params=pltpu.CompilerParams(vmem_limit_bytes=40 << 20),
        name="down",
    )(hidden, *held[2], flat_weight)

    returned = lax.all_to_all(
        expert_rows.reshape(expert_count, capacity, chunks, LANES), ("pair", "yl"), 0, 0, tiled=True
    )
    return pl.pallas_call(
        functools.partial(combine_kernel, quarter, model_width, top_count),
        out_shape=jax.ShapeDtypeStruct((quarter, model_width), jnp.bfloat16),
        in_specs=[SMEM, SMEM, VMEM, VMEM],
        out_specs=VMEM,
        scratch_shapes=[pltpu.VMEM((quarter * chunks, LANES), jnp.float32)],
        compiler_params=pltpu.CompilerParams(vmem_limit_bytes=30 << 20),
        name="combine",
    )(places, flat_weight, returned.reshape(slots, chunks, LANES), mixed_rows)


def solution(mesh):
    split = Mesh(mesh.devices.reshape(mesh.shape["sp"] // 2, 2, mesh.shape["tp"] // 2, 2), ALL)
    in_specs = (
        P(ALL, None),
        P(SP, TP),
        P(SP),
        P(TP, None, None),
        P(TP),
        P(TP, None),
        P(),
        P(SP, None),
        P(ALL, None),
        P(SP, None, TP),
        P(SP, None, TP),
        P(SP, TP, None),
    )
    return jax.shard_map(forward, mesh=split, in_specs=in_specs, out_specs=P(ALL, None), check_vma=False)
```

```python
import functools

import jax
import jax.numpy as jnp
from jax import lax
from jax.experimental import pallas as pl
from jax.experimental.pallas import tpu as pltpu
from jax.sharding import Mesh, PartitionSpec as P

SPAN = 16
EPS = 1e-06
LANES = 128


VMEM = pl.BlockSpec(memory_space=pltpu.VMEM)
SMEM = pl.BlockSpec(memory_space=pltpu.SMEM)
HBM = pl.BlockSpec(memory_space=pltpu.HBM)


def tile_rows(rows, chunk):
    return pl.ds(chunk // 8 * rows * 8 + chunk % 8, rows, stride=8)


def spread(wide, rows, chunks, value):
    tall = value.astype(jnp.float32).reshape(rows, chunks, LANES)
    for part in range(chunks // 8):
        wide[part * rows * 8 : (part + 1) * rows * 8] = tall[:, part * 8 : part * 8 + 8].reshape(rows * 8, LANES)


def gathered(wide, rows, chunks):
    parts = [wide[part * rows * 8 : (part + 1) * rows * 8].reshape(rows, 8, LANES) for part in range(chunks // 8)]
    return jnp.concatenate(parts, axis=1).astype(jnp.bfloat16)


def mix_kernel(rows, reach, pool_ref, docs_ref, prior_ref, map_ref, scale_ref, weight_ref, *refs):
    own_ref, far_plus, far_minus, next_low, next_high, prev_low, prev_high = refs[:7]
    data, docs, tally, turned = refs[7:]
    width = pool_ref.shape[1]
    tp = lax.axis_index(TP)
    window = jnp.left_shift(jnp.int32(2), tp)
    first = (lax.axis_index(SP) == 0).astype(jnp.float32)
    data[:reach] = jnp.zeros((reach, width), jnp.float32)
    data[reach : 2 * reach] = prior_ref[:, :width].astype(jnp.float32)
    data[2 * reach :] = pool_ref[...].astype(jnp.float32)
    docs[:reach] = jnp.full((reach, LANES), -1.0, jnp.float32)
    docs[reach : 2 * reach] = prior_ref[:, width:].astype(jnp.float32) * (1.0 - first) - first
    docs[2 * reach :] = docs_ref[...].astype(jnp.float32)
    tally[...] = jnp.ones(tally.shape, jnp.float32)
    extent = rows + reach
    span = 1
    while span < reach:
        @pl.when(span < window)
        def _():
            same = docs[reach:] == docs[reach - span : reach - span + extent]
            wide_same = jnp.concatenate([same] * (width // LANES), axis=1)
            grown = data[reach:] + jnp.where(wide_same, data[reach - span : reach - span + extent], 0.0)
            counted = tally[reach:] + jnp.where(same, tally[reach - span : reach - span + extent], 0.0)
            data[reach:] = grown
            tally[reach:] = counted

        span *= 2
    count = jnp.concatenate([tally[2 * reach :]] * (width // LANES), axis=1)
    pooled = (data[2 * reach :] / count - pool_ref[...].astype(jnp.float32)).astype(jnp.bfloat16)
    branch = (jnp.dot(pooled, map_ref[0], preferred_element_type=jnp.float32) * scale_ref[...]).astype(jnp.bfloat16)
    quarter = rows // 4
    turned[...] = branch
    order = [turned[pl.ds(lax.rem(tp + step, 4) * quarter, quarter), :] for step in range(4)]
    lined = jnp.concatenate(order, axis=0)
    half = weight_ref.shape[1] // 2
    low = jnp.dot(lined, weight_ref[:, :half], preferred_element_type=jnp.float32).astype(jnp.bfloat16)
    own_ref[:, :half] = low[:quarter]
    next_low[...] = low[quarter : 2 * quarter]
    far_minus[...] = low[2 * quarter : 3 * quarter]
    prev_low[...] = low[3 * quarter :]
    high = jnp.dot(lined, weight_ref[:, half:], preferred_element_type=jnp.float32).astype(jnp.bfloat16)
    own_ref[:, half:] = high[:quarter]
    next_high[...] = high[quarter : 2 * quarter]
    far_plus[...] = high[2 * quarter : 3 * quarter]
    prev_high[...] = high[3 * quarter :]


def dispatch_kernel(rows, width, slots, tok_ref, own_ref, nl_ref, nh_ref, pl_ref, ph_ref, stream_ref, gain_ref, out_ref, mixed_ref, wide, tiles):
    chunks = width // LANES
    low = nl_ref[...].astype(jnp.float32) + pl_ref[...].astype(jnp.float32)
    high = nh_ref[...].astype(jnp.float32) + ph_ref[...].astype(jnp.float32)
    total = own_ref[...].astype(jnp.float32) + jnp.concatenate([low, high], axis=1)
    mixed = (stream_ref[...].astype(jnp.float32) + total).astype(jnp.bfloat16)
    mixed_ref[...] = mixed
    up = mixed.astype(jnp.float32)
    scale = lax.rsqrt(jnp.sum(up * up, axis=1, keepdims=True) * (1.0 / width) + EPS)
    for chunk in range(chunks):
        cols = slice(chunk * LANES, (chunk + 1) * LANES)
        piece = up[:, cols] * scale * gain_ref[:, cols]
        wide[tile_rows(rows, chunk), :] = piece
    tiles[...] = gathered(wide, rows, chunks)

    @pl.loop(0, slots, unroll=8)
    def _(slot):
        out_ref[slot] = tiles[tok_ref[slot]]


def expert_kernel(rows, width, ff, half, x_ref, *refs):
    own, swapped, near, both, last = [refs[3 * i : 3 * i + 3] for i in range(5)]
    out_ref, wide, flat, hidden, gates, ups, downs, sems = refs[16:]
    chunks = width // LANES
    is_home = half()
    home_side = (own, near, both, swapped)
    away_side = (last, near, both, swapped)
    targets = (gates, ups, downs)

    def copy_in(side, place, j):
        return pltpu.make_async_copy(side[place][j], targets[j].at[place], sems.at[j, place])

    for place, j in [(place, j) for place in range(4) for j in range(2)] + [(place, 2) for place in range(4)]:
        if home_side[place] is away_side[place]:
            copy_in(home_side, place, j).start()
        else:
            @pl.when(is_home)
            def _():
                copy_in(home_side, place, j).start()

            @pl.when(jnp.logical_not(is_home))
            def _():
                copy_in(away_side, place, j).start()

    spread(wide, rows, chunks, x_ref[...])
    for chunk in range(chunks):
        flat[:, chunk * LANES : (chunk + 1) * LANES] = wide[tile_rows(rows, chunk), :].astype(jnp.bfloat16)

    for place in range(4):
        copy_in(home_side, place, 0).wait()
        copy_in(home_side, place, 1).wait()
        gate_pre = jnp.dot(flat[...], gates[place], preferred_element_type=jnp.float32)
        up_pre = jnp.dot(flat[...], ups[place], preferred_element_type=jnp.float32)
        product = gate_pre / (1.0 + jnp.exp(-gate_pre)) * up_pre
        hidden[:, place * ff : (place + 1) * ff] = product.astype(jnp.bfloat16)

    for place in range(4):
        copy_in(home_side, place, 2).wait()
    step = 4 * LANES
    weights = downs.reshape(4 * ff, width)
    for begin in range(0, width, step):
        total = jnp.dot(hidden[...], weights[:, begin : begin + step], preferred_element_type=jnp.float32)
        for piece in range(step // LANES):
            wide[tile_rows(rows, begin // LANES + piece), :] = total[:, piece * LANES : (piece + 1) * LANES]
    out_ref[...] = gathered(wide, rows, chunks)


def combine_kernel(rows, width, top, pos_ref, weight_ref, got_ref, mixed_ref, out_ref, wide):
    chunks = width // LANES

    @pl.loop(0, rows, unroll=4)
    def _(row):
        total = weight_ref[row * top] * got_ref[pos_ref[row * top]].astype(jnp.float32)
        for k in range(1, top):
            total = total + weight_ref[row * top + k] * got_ref[pos_ref[row * top + k]].astype(jnp.float32)
        for part in range(chunks // 8):
            wide[pl.ds(pl.multiple_of(part * rows * 8 + row * 8, 8), 8), :] = total[part * 8 : part * 8 + 8]

    for chunk in range(chunks):
        cols = slice(chunk * LANES, (chunk + 1) * LANES)
        piece = wide[tile_rows(rows, chunk), :]
        out_ref[:, cols] = (mixed_ref[:, cols].astype(jnp.float32) + piece).astype(jnp.bfloat16)


def slot_tables(route_block, expert_count, capacity, top_count, flip):
    flattened = route_block.reshape(-1)
    one_hot = (flattened[:, None] == jnp.arange(expert_count, dtype=jnp.int32)[None, :]).astype(jnp.int32)
    ranking = jnp.sum((jnp.cumsum(one_hot, axis=0) - one_hot) * one_hot, axis=1)
    place = (flattened // 2 * 2 + (flattened + flip) % 2) * capacity + ranking
    matches = place[None, :] == jnp.arange(expert_count * capacity, dtype=jnp.int32)[:, None]
    sources = jnp.sum(jnp.where(matches, jnp.arange(flattened.shape[0], dtype=jnp.int32)[None, :], 0), axis=1)
    return place, sources // top_count


def weight_moves(sp_count, tp_count):
    def at(pair, core, y):
        return (2 * pair + core) * tp_count + y

    served = lambda y: (y % 2 + y // 2) % 2
    home = lambda p, y: at(p, served(y), y)
    away = lambda p, y: at(p, 1 - served(y), y)
    inner = lambda y: tp_count - 1 - y
    outer = lambda y: y + 1 - 2 * (y % 2)
    pairs = [(pair, y) for pair in range(sp_count // 2) for y in range(tp_count)]
    over = [(home(p, y), away(p, y)) for p, y in pairs]
    back = [(away(p, y), home(p, y)) for p, y in pairs]
    near = [(home(p, y), home(p, inner(y))) for p, y in pairs] + [(away(p, y), away(p, outer(y))) for p, y in pairs]
    relay = [(away(p, y), home(p, inner(y))) for p, y in pairs] + over
    return near, relay, over, back


ALL = ("pair", "core", "yh", "yl")
SP = ("pair", "core")
TP = ("yh", "yl")


def forward(
    stream,
    pool_in,
    doc_ids,
    pool_map,
    pool_scale,
    out_weight,
    norm_gain,
    routes,
    route_weight,
    expert_gate,
    expert_up,
    expert_down,
):
    row_count = pool_in.shape[0]
    model_width = stream.shape[1]
    top_count = routes.shape[1]
    tp_count = lax.axis_size(TP)
    expert_count = lax.axis_size(SP)
    quarter = row_count // tp_count
    capacity = max(2, 3 * top_count * quarter // (2 * expert_count))
    slots = expert_count * capacity
    chunks = model_width // LANES
    tp_index = lax.axis_index(TP)
    docs = jnp.broadcast_to(doc_ids.astype(jnp.bfloat16)[:, None], (row_count, LANES))
    tail = jnp.concatenate([pool_in[row_count - SPAN :], docs[row_count - SPAN :]], axis=1)
    prior = lax.ppermute(tail, SP, [(i, i + 1) for i in range(expert_count - 1)])
    piece = jax.ShapeDtypeStruct((quarter, model_width // 2), jnp.bfloat16)
    held_rows, far_plus, far_minus, next_low, next_high, prev_low, prev_high = pl.pallas_call(
        functools.partial(mix_kernel, row_count, SPAN),
        out_shape=(jax.ShapeDtypeStruct((quarter, model_width), jnp.bfloat16),) + (piece,) * 6,
        in_specs=[VMEM] * 6,
        out_specs=(VMEM,) * 7,
        scratch_shapes=[
            pltpu.VMEM((row_count + 2 * SPAN, pool_in.shape[1]), jnp.float32),
            pltpu.VMEM((row_count + 2 * SPAN, LANES), jnp.float32),
            pltpu.VMEM((row_count + 2 * SPAN, LANES), jnp.float32),
            pltpu.VMEM((row_count, out_weight.shape[0]), jnp.bfloat16),
        ],
        name="mix",
    )(pool_in, docs, prior, pool_map, pool_scale[None], out_weight)

    own = (expert_gate[0], expert_up[0], expert_down[0])
    near, relay, over, back = weight_moves(expert_count, tp_count)
    plus = [(y, (y + 1) % tp_count) for y in range(tp_count)]
    minus = [(y, (y - 1) % tp_count) for y in range(tp_count)]

    def pass_on(array, pairs):
        return lax.ppermute(array, TP, pairs)

    def joined(left, right):
        return (left.astype(jnp.float32) + right.astype(jnp.float32)).astype(jnp.bfloat16)

    from_low = pass_on(far_plus, plus)
    from_high = pass_on(far_minus, minus)
    got_next_low = pass_on(next_low, plus)
    got_prev_high = pass_on(prev_high, minus)
    got_next_high = pass_on(joined(next_high, from_low), plus)
    got_prev_low = pass_on(joined(prev_low, from_high), minus)
    is_home = lambda: lax.axis_index("core") == (lax.axis_index("yl") + lax.axis_index("yh")) % 2
    held = []
    for array in own:
        first = lax.ppermute(array, ALL, near)
        second = lax.ppermute(first, ALL, relay)
        swapped = lax.ppermute(jnp.where(is_home(), array, first), ALL, over + back)
        last = lax.ppermute(second, ALL, over)
        held.append((array, swapped, first, second, last))

    own_routes = lax.dynamic_slice_in_dim(routes, tp_index * quarter, quarter, 0)
    places, tokens = slot_tables(own_routes, expert_count, capacity, top_count, lax.axis_index("yh"))

    dispatch, mixed_rows = pl.pallas_call(
        functools.partial(dispatch_kernel, quarter, model_width, slots),
        out_shape=(
            jax.ShapeDtypeStruct((slots, chunks, LANES), jnp.bfloat16),
            jax.ShapeDtypeStruct((quarter, model_width), jnp.bfloat16),
        ),
        in_specs=[SMEM] + [VMEM] * 7,
        out_specs=(VMEM, VMEM),
        scratch_shapes=[
            pltpu.VMEM((quarter * chunks, LANES), jnp.float32),
            pltpu.VMEM((quarter, chunks, LANES), jnp.bfloat16),
        ],
        name="dispatch",
    )(tokens, held_rows, got_next_low, got_next_high, got_prev_low, got_prev_high, stream, norm_gain[None])

    send = dispatch.reshape(expert_count, capacity, chunks, LANES)
    arrived = lax.all_to_all(send, ("pair", "yl"), 0, 0, tiled=True)

    ff = expert_gate.shape[2]
    flat_weight = route_weight.reshape(-1)
    expert_rows = pl.pallas_call(
        functools.partial(expert_kernel, slots, model_width, ff, is_home),
        out_shape=jax.ShapeDtypeStruct((slots, chunks, LANES), jnp.bfloat16),
        in_specs=[VMEM] + [HBM] * 15 + [SMEM],
        out_specs=VMEM,
        scratch_shapes=[
            pltpu.VMEM((slots * chunks, LANES), jnp.float32),
            pltpu.VMEM((slots, model_width), jnp.bfloat16),
            pltpu.VMEM((slots, ff * tp_count), jnp.bfloat16),
            pltpu.VMEM((tp_count, model_width, ff), jnp.bfloat16),
            pltpu.VMEM((tp_count, model_width, ff), jnp.bfloat16),
            pltpu.VMEM((tp_count, ff, model_width), jnp.bfloat16),
            pltpu.SemaphoreType.DMA((3, tp_count)),
        ],
        compiler_params=pltpu.CompilerParams(vmem_limit_bytes=32 << 20),
        name="experts",
    )(arrived.reshape(slots * chunks, LANES), *[h[i] for i in range(5) for h in held], flat_weight)

    returned = lax.all_to_all(
        expert_rows.reshape(expert_count, capacity, chunks, LANES), ("pair", "yl"), 0, 0, tiled=True
    )
    return pl.pallas_call(
        functools.partial(combine_kernel, quarter, model_width, top_count),
        out_shape=jax.ShapeDtypeStruct((quarter, model_width), jnp.bfloat16),
        in_specs=[SMEM, SMEM, VMEM, VMEM],
        out_specs=VMEM,
        scratch_shapes=[pltpu.VMEM((quarter * chunks, LANES), jnp.float32)],
        compiler_params=pltpu.CompilerParams(vmem_limit_bytes=30 << 20),
        name="combine",
    )(places, flat_weight, returned.reshape(slots, chunks, LANES), mixed_rows)


def solution(mesh):
    split = Mesh(mesh.devices.reshape(mesh.shape["sp"] // 2, 2, mesh.shape["tp"] // 2, 2), ALL)
    in_specs = (
        P(ALL, None),
        P(SP, TP),
        P(SP),
        P(TP, None, None),
        P(TP),
        P(TP, None),
        P(),
        P(SP, None),
        P(ALL, None),
        P(SP, None, TP),
        P(SP, None, TP),
        P(SP, TP, None),
    )
    return jax.shard_map(forward, mesh=split, in_specs=in_specs, out_specs=P(ALL, None), check_vma=False)
```

```python
import functools

import jax
import jax.numpy as jnp
from jax import lax
from jax.experimental import pallas as pl
from jax.experimental.pallas import tpu as pltpu
from jax.sharding import Mesh, PartitionSpec as P

SPAN = 16
EPS = 1e-06
LANES = 128


VMEM = pl.BlockSpec(memory_space=pltpu.VMEM)
SMEM = pl.BlockSpec(memory_space=pltpu.SMEM)
HBM = pl.BlockSpec(memory_space=pltpu.HBM)


def tile_rows(rows, chunk):
    return pl.ds(chunk // 8 * rows * 8 + chunk % 8, rows, stride=8)


def spread(wide, rows, chunks, value):
    tall = value.astype(jnp.float32).reshape(rows, chunks, LANES)
    for part in range(chunks // 8):
        wide[part * rows * 8 : (part + 1) * rows * 8] = tall[:, part * 8 : part * 8 + 8].reshape(rows * 8, LANES)


def gathered(wide, rows, chunks):
    parts = [wide[part * rows * 8 : (part + 1) * rows * 8].reshape(rows, 8, LANES) for part in range(chunks // 8)]
    return jnp.concatenate(parts, axis=1).astype(jnp.bfloat16)


def mix_kernel(rows, reach, pool_ref, docs_ref, prior_ref, map_ref, scale_ref, weight_ref, *refs):
    own_ref, far_plus, far_minus, next_low, next_high, prev_low, prev_high = refs[:7]
    data, docs, tally, turned = refs[7:]
    width = pool_ref.shape[1]
    tp = lax.axis_index(TP)
    window = jnp.left_shift(jnp.int32(2), tp)
    first = (lax.axis_index(SP) == 0).astype(jnp.float32)
    data[:reach] = jnp.zeros((reach, width), jnp.float32)
    data[reach : 2 * reach] = prior_ref[:, :width].astype(jnp.float32)
    data[2 * reach :] = pool_ref[...].astype(jnp.float32)
    docs[:reach] = jnp.full((reach, LANES), -1.0, jnp.float32)
    docs[reach : 2 * reach] = prior_ref[:, width:].astype(jnp.float32) * (1.0 - first) - first
    docs[2 * reach :] = docs_ref[...].astype(jnp.float32)
    tally[...] = jnp.ones(tally.shape, jnp.float32)
    extent = rows + reach
    span = 1
    while span < reach:
        @pl.when(span < window)
        def _():
            same = docs[reach:] == docs[reach - span : reach - span + extent]
            wide_same = jnp.concatenate([same] * (width // LANES), axis=1)
            grown = data[reach:] + jnp.where(wide_same, data[reach - span : reach - span + extent], 0.0)
            counted = tally[reach:] + jnp.where(same, tally[reach - span : reach - span + extent], 0.0)
            data[reach:] = grown
            tally[reach:] = counted

        span *= 2
    count = jnp.concatenate([tally[2 * reach :]] * (width // LANES), axis=1)
    pooled = (data[2 * reach :] / count - pool_ref[...].astype(jnp.float32)).astype(jnp.bfloat16)
    branch = (jnp.dot(pooled, map_ref[0], preferred_element_type=jnp.float32) * scale_ref[...]).astype(jnp.bfloat16)
    quarter = rows // 4
    turned[...] = branch
    order = [turned[pl.ds(lax.rem(tp + step, 4) * quarter, quarter), :] for step in range(4)]
    lined = jnp.concatenate(order, axis=0)
    half = weight_ref.shape[1] // 2
    low = jnp.dot(lined, weight_ref[:, :half], preferred_element_type=jnp.float32).astype(jnp.bfloat16)
    own_ref[:, :half] = low[:quarter]
    next_low[...] = low[quarter : 2 * quarter]
    far_minus[...] = low[2 * quarter : 3 * quarter]
    prev_low[...] = low[3 * quarter :]
    high = jnp.dot(lined, weight_ref[:, half:], preferred_element_type=jnp.float32).astype(jnp.bfloat16)
    own_ref[:, half:] = high[:quarter]
    next_high[...] = high[quarter : 2 * quarter]
    far_plus[...] = high[2 * quarter : 3 * quarter]
    prev_high[...] = high[3 * quarter :]


def dispatch_kernel(rows, width, slots, tok_ref, own_ref, nl_ref, nh_ref, pl_ref, ph_ref, stream_ref, gain_ref, out_ref, mixed_ref, wide, tiles):
    chunks = width // LANES
    low = nl_ref[...].astype(jnp.float32) + pl_ref[...].astype(jnp.float32)
    high = nh_ref[...].astype(jnp.float32) + ph_ref[...].astype(jnp.float32)
    total = own_ref[...].astype(jnp.float32) + jnp.concatenate([low, high], axis=1)
    mixed = (stream_ref[...].astype(jnp.float32) + total).astype(jnp.bfloat16)
    mixed_ref[...] = mixed
    up = mixed.astype(jnp.float32)
    scale = lax.rsqrt(jnp.sum(up * up, axis=1, keepdims=True) * (1.0 / width) + EPS)
    for chunk in range(chunks):
        cols = slice(chunk * LANES, (chunk + 1) * LANES)
        piece = up[:, cols] * scale * gain_ref[:, cols]
        wide[tile_rows(rows, chunk), :] = piece
    tiles[...] = gathered(wide, rows, chunks)

    @pl.loop(0, slots, unroll=8)
    def _(slot):
        out_ref[slot] = tiles[tok_ref[slot]]


def start_copies(is_home, home_side, away_side, copy_in, indices):
    for place in range(4):
        for j in indices:
            if home_side[place] is away_side[place]:
                copy_in(home_side, place, j).start()
            else:
                @pl.when(is_home)
                def _():
                    copy_in(home_side, place, j).start()

                @pl.when(jnp.logical_not(is_home))
                def _():
                    copy_in(away_side, place, j).start()


def hidden_kernel(rows, width, ff, half, x_ref, *refs):
    own, swapped, near, both, last = [refs[2 * i : 2 * i + 2] for i in range(5)]
    out_ref, wide, flat, gates, ups, sems = refs[10:]
    chunks = width // LANES
    home_side = (own, near, both, swapped)
    away_side = (last, near, both, swapped)
    targets = (gates, ups)

    def copy_in(side, place, j):
        return pltpu.make_async_copy(side[place][j], targets[j].at[place], sems.at[j, place])

    start_copies(half(), home_side, away_side, copy_in, (0, 1))
    spread(wide, rows, chunks, x_ref[...])
    for chunk in range(chunks):
        flat[:, chunk * LANES : (chunk + 1) * LANES] = wide[tile_rows(rows, chunk), :].astype(jnp.bfloat16)

    for place in range(4):
        copy_in(home_side, place, 0).wait()
        copy_in(home_side, place, 1).wait()
        gate_pre = jnp.dot(flat[...], gates[place], preferred_element_type=jnp.float32)
        up_pre = jnp.dot(flat[...], ups[place], preferred_element_type=jnp.float32)
        product = gate_pre / (1.0 + jnp.exp(-gate_pre)) * up_pre
        out_ref[:, place * ff : (place + 1) * ff] = product.astype(jnp.bfloat16)


def down_kernel(rows, width, ff, half, hidden_ref, own, swapped, near, both, last, after_ref, out_ref, wide, downs, sems):
    chunks = width // LANES
    home_side = ((own,), (near,), (both,), (swapped,))
    away_side = ((last,), home_side[1], home_side[2], home_side[3])

    def copy_in(side, place, j):
        return pltpu.make_async_copy(side[place][j], downs.at[pl.ds(place * ff, ff)], sems.at[place])

    start_copies(half(), home_side, away_side, copy_in, (0,))
    for place in range(4):
        copy_in(home_side, place, 0).wait()
    step = 4 * LANES
    for begin in range(0, width, step):
        total = jnp.dot(hidden_ref[...], downs[:, begin : begin + step], preferred_element_type=jnp.float32)
        for piece in range(step // LANES):
            wide[tile_rows(rows, begin // LANES + piece), :] = total[:, piece * LANES : (piece + 1) * LANES]
    out_ref[...] = gathered(wide, rows, chunks)


def combine_kernel(rows, width, top, pos_ref, weight_ref, got_ref, mixed_ref, out_ref, wide):
    chunks = width // LANES

    @pl.loop(0, rows, unroll=4)
    def _(row):
        total = weight_ref[row * top] * got_ref[pos_ref[row * top]].astype(jnp.float32)
        for k in range(1, top):
            total = total + weight_ref[row * top + k] * got_ref[pos_ref[row * top + k]].astype(jnp.float32)
        for part in range(chunks // 8):
            wide[pl.ds(pl.multiple_of(part * rows * 8 + row * 8, 8), 8), :] = total[part * 8 : part * 8 + 8]

    for chunk in range(chunks):
        cols = slice(chunk * LANES, (chunk + 1) * LANES)
        piece = wide[tile_rows(rows, chunk), :]
        out_ref[:, cols] = (mixed_ref[:, cols].astype(jnp.float32) + piece).astype(jnp.bfloat16)


def slot_tables(route_block, expert_count, capacity, top_count, flip):
    flattened = route_block.reshape(-1)
    one_hot = (flattened[:, None] == jnp.arange(expert_count, dtype=jnp.int32)[None, :]).astype(jnp.int32)
    ranking = jnp.sum((jnp.cumsum(one_hot, axis=0) - one_hot) * one_hot, axis=1)
    place = (flattened // 2 * 2 + (flattened + flip) % 2) * capacity + ranking
    matches = place[None, :] == jnp.arange(expert_count * capacity, dtype=jnp.int32)[:, None]
    sources = jnp.sum(jnp.where(matches, jnp.arange(flattened.shape[0], dtype=jnp.int32)[None, :], 0), axis=1)
    return place, sources // top_count


def weight_moves(sp_count, tp_count):
    def at(pair, core, y):
        return (2 * pair + core) * tp_count + y

    served = lambda y: (y % 2 + y // 2) % 2
    home = lambda p, y: at(p, served(y), y)
    away = lambda p, y: at(p, 1 - served(y), y)
    inner = lambda y: tp_count - 1 - y
    outer = lambda y: y + 1 - 2 * (y % 2)
    pairs = [(pair, y) for pair in range(sp_count // 2) for y in range(tp_count)]
    over = [(home(p, y), away(p, y)) for p, y in pairs]
    back = [(away(p, y), home(p, y)) for p, y in pairs]
    near = [(home(p, y), home(p, inner(y))) for p, y in pairs] + [(away(p, y), away(p, outer(y))) for p, y in pairs]
    relay = [(away(p, y), home(p, inner(y))) for p, y in pairs] + over
    return near, relay, over, back


ALL = ("pair", "core", "yh", "yl")
SP = ("pair", "core")
TP = ("yh", "yl")


def forward(
    stream,
    pool_in,
    doc_ids,
    pool_map,
    pool_scale,
    out_weight,
    norm_gain,
    routes,
    route_weight,
    expert_gate,
    expert_up,
    expert_down,
):
    row_count = pool_in.shape[0]
    model_width = stream.shape[1]
    top_count = routes.shape[1]
    tp_count = lax.axis_size(TP)
    expert_count = lax.axis_size(SP)
    quarter = row_count // tp_count
    capacity = max(2, 3 * top_count * quarter // (2 * expert_count))
    slots = expert_count * capacity
    chunks = model_width // LANES
    tp_index = lax.axis_index(TP)
    docs = jnp.broadcast_to(doc_ids.astype(jnp.bfloat16)[:, None], (row_count, LANES))
    tail = jnp.concatenate([pool_in[row_count - SPAN :], docs[row_count - SPAN :]], axis=1)
    prior = lax.ppermute(tail, SP, [(i, i + 1) for i in range(expert_count - 1)])
    piece = jax.ShapeDtypeStruct((quarter, model_width // 2), jnp.bfloat16)
    held_rows, far_plus, far_minus, next_low, next_high, prev_low, prev_high = pl.pallas_call(
        functools.partial(mix_kernel, row_count, SPAN),
        out_shape=(jax.ShapeDtypeStruct((quarter, model_width), jnp.bfloat16),) + (piece,) * 6,
        in_specs=[VMEM] * 6,
        out_specs=(VMEM,) * 7,
        scratch_shapes=[
            pltpu.VMEM((row_count + 2 * SPAN, pool_in.shape[1]), jnp.float32),
            pltpu.VMEM((row_count + 2 * SPAN, LANES), jnp.float32),
            pltpu.VMEM((row_count + 2 * SPAN, LANES), jnp.float32),
            pltpu.VMEM((row_count, out_weight.shape[0]), jnp.bfloat16),
        ],
        name="mix",
    )(pool_in, docs, prior, pool_map, pool_scale[None], out_weight)

    own = (expert_gate[0], expert_up[0], expert_down[0])
    near, relay, over, back = weight_moves(expert_count, tp_count)
    plus = [(y, (y + 1) % tp_count) for y in range(tp_count)]
    minus = [(y, (y - 1) % tp_count) for y in range(tp_count)]

    def pass_on(array, pairs):
        return lax.ppermute(array, TP, pairs)

    def joined(left, right):
        return (left.astype(jnp.float32) + right.astype(jnp.float32)).astype(jnp.bfloat16)

    from_low = pass_on(far_plus, plus)
    from_high = pass_on(far_minus, minus)
    got_next_low = pass_on(next_low, plus)
    got_prev_high = pass_on(prev_high, minus)
    got_next_high = pass_on(joined(next_high, from_low), plus)
    got_prev_low = pass_on(joined(prev_low, from_high), minus)
    is_home = lambda: lax.axis_index("core") == (lax.axis_index("yl") + lax.axis_index("yh")) % 2
    held = []
    for array in own:
        first = lax.ppermute(array, ALL, near)
        second = lax.ppermute(first, ALL, relay)
        swapped = lax.ppermute(jnp.where(is_home(), array, first), ALL, over + back)
        last = lax.ppermute(second, ALL, over)
        held.append((array, swapped, first, second, last))

    own_routes = lax.dynamic_slice_in_dim(routes, tp_index * quarter, quarter, 0)
    places, tokens = slot_tables(own_routes, expert_count, capacity, top_count, lax.axis_index("yh"))

    dispatch, mixed_rows = pl.pallas_call(
        functools.partial(dispatch_kernel, quarter, model_width, slots),
        out_shape=(
            jax.ShapeDtypeStruct((slots, chunks, LANES), jnp.bfloat16),
            jax.ShapeDtypeStruct((quarter, model_width), jnp.bfloat16),
        ),
        in_specs=[SMEM] + [VMEM] * 7,
        out_specs=(VMEM, VMEM),
        scratch_shapes=[
            pltpu.VMEM((quarter * chunks, LANES), jnp.float32),
            pltpu.VMEM((quarter, chunks, LANES), jnp.bfloat16),
        ],
        name="dispatch",
    )(tokens, held_rows, got_next_low, got_next_high, got_prev_low, got_prev_high, stream, norm_gain[None])

    send = dispatch.reshape(expert_count, capacity, chunks, LANES)
    arrived = lax.all_to_all(send, ("pair", "yl"), 0, 0, tiled=True)

    ff = expert_gate.shape[2]
    flat_weight = route_weight.reshape(-1)
    hidden = pl.pallas_call(
        functools.partial(hidden_kernel, slots, model_width, ff, is_home),
        out_shape=jax.ShapeDtypeStruct((slots, ff * tp_count), jnp.bfloat16),
        in_specs=[VMEM] + [HBM] * 10,
        out_specs=VMEM,
        scratch_shapes=[
            pltpu.VMEM((slots * chunks, LANES), jnp.float32),
            pltpu.VMEM((slots, model_width), jnp.bfloat16),
            pltpu.VMEM((tp_count, model_width, ff), jnp.bfloat16),
            pltpu.VMEM((tp_count, model_width, ff), jnp.bfloat16),
            pltpu.SemaphoreType.DMA((2, tp_count)),
        ],
        compiler_params=pltpu.CompilerParams(vmem_limit_bytes=24 << 20),
        name="hidden",
    )(arrived.reshape(slots * chunks, LANES), *[h[i] for i in range(5) for h in held[:2]])
    expert_rows = pl.pallas_call(
        functools.partial(down_kernel, slots, model_width, ff, is_home),
        out_shape=jax.ShapeDtypeStruct((slots, chunks, LANES), jnp.bfloat16),
        in_specs=[VMEM] + [HBM] * 5 + [SMEM],
        out_specs=VMEM,
        scratch_shapes=[
            pltpu.VMEM((slots * chunks, LANES), jnp.float32),
            pltpu.VMEM((ff * tp_count, model_width), jnp.bfloat16),
            pltpu.SemaphoreType.DMA((tp_count,)),
        ],
        compiler_params=pltpu.CompilerParams(vmem_limit_bytes=24 << 20),
        name="down",
    )(hidden, *held[2], flat_weight)

    returned = lax.all_to_all(
        expert_rows.reshape(expert_count, capacity, chunks, LANES), ("pair", "yl"), 0, 0, tiled=True
    )
    return pl.pallas_call(
        functools.partial(combine_kernel, quarter, model_width, top_count),
        out_shape=jax.ShapeDtypeStruct((quarter, model_width), jnp.bfloat16),
        in_specs=[SMEM, SMEM, VMEM, VMEM],
        out_specs=VMEM,
        scratch_shapes=[pltpu.VMEM((quarter * chunks, LANES), jnp.float32)],
        compiler_params=pltpu.CompilerParams(vmem_limit_bytes=30 << 20),
        name="combine",
    )(places, flat_weight, returned.reshape(slots, chunks, LANES), mixed_rows)


def solution(mesh):
    split = Mesh(mesh.devices.reshape(mesh.shape["sp"] // 2, 2, mesh.shape["tp"] // 2, 2), ALL)
    in_specs = (
        P(ALL, None),
        P(SP, TP),
        P(SP),
        P(TP, None, None),
        P(TP),
        P(TP, None),
        P(),
        P(SP, None),
        P(ALL, None),
        P(SP, None, TP),
        P(SP, None, TP),
        P(SP, TP, None),
    )
    return jax.shard_map(forward, mesh=split, in_specs=in_specs, out_specs=P(ALL, None), check_vma=False)
```
